32 devices in a mesh: sp: 8 (over z, y), tp: 4 (over x, core).
Axes of the slice: x: 2, y: 2, z: 4, core: 2. Of those that a mesh axis runs over, the one named last changes fastest.
Arguments:
- queries: bfloat16 [1536, 1024], P('sp', 'tp'), may hold values from -0.75 to 0.75
- key_vectors: bfloat16 [1536, 1024], P('sp', 'tp'), may hold values from -0.75 to 0.75
- values_in: bfloat16 [1536, 2048], P('sp', 'tp'), may hold values from -0.75 to 0.75
- log_decay: float32 [1536, 1024], P('sp', 'tp'), may hold values from -1 to 0
- mixed_heads: bfloat16 [1536, 2048], P('sp', 'tp'), may hold values from -6 to 6
- out_proj: bfloat16 [2048, 2048], P('tp'), may hold values from -0.125 to 0.125
- layer_input: bfloat16 [1536, 2048], P('sp'), may hold values from -6 to 6
- cotangent: bfloat16 [1536, 2048], P('sp'), may hold values from -6 to 6
- routes: int32 [1536, 2], P('sp'), may hold values from 0 to 15, all different within a row; in each aligned block of 192 rows (0 to 191, 192 to 383, ...) at most 48 rows name the same one
- route_weight: float32 [1536, 2], P('sp'), may hold values from 0.25 to 2
- gate_weight: bfloat16 [16, 2048, 1024], P('sp', None, 'tp'), may hold values from -0.125 to 0.125
- up_weight: bfloat16 [16, 2048, 1024], P('sp', None, 'tp'), may hold values from -0.125 to 0.125
- down_weight: bfloat16 [16, 1024, 2048], P('sp', 'tp'), may hold values from -0.1875 to 0.1875
Outputs:
- grad_gate: float32 [16, 2048, 1024], P('sp', None, 'tp')
- grad_up: float32 [16, 2048, 1024], P('sp', None, 'tp')
- grad_down: float32 [16, 1024, 2048], P('sp', 'tp')
- grad_proj: float32 [2048, 2048], P('sp', 'tp')
- grad_query: float32 [1536, 1024], P('sp', 'tp')
- grad_key: float32 [1536, 1024], P('sp', 'tp')
- grad_value: float32 [1536, 2048], P('sp', 'tp')
- grad_decay: float32 [1536, 1024], P('sp', 'tp')
The draws below stay inside these ranges and needn't reach their ends.
Inputs may be any that keep to these rules, and one draw needn't show every extreme that they name: `routes`: in each aligned block of 192 tokens no expert is named by more than 48 pairs, and in some block one expert is named by exactly 48 pairs; the 2 experts of a token differ.
All inputs are finite; a program needn't handle non-finite values.
Results may differ from the reference program's by a relative error of at most 0.015.
Values may be sent and summed in bfloat16 or wider, within the bound.
A program may use at most 192 MiB of HBM per device.

```python
import math
import jax
import jax.numpy as jnp
import numpy as np
from jax import lax

D = 2048
HEADS = 8
DK = 128
DV = 256
FE = 1024
TOP = 2
TOK_DEV = 192
EXPERTS = 16
STREAM_LENGTH = 1536
CAP = 48
N_TP = 4


def draw_log_decay(key, part):
    lookup_entries = jax.random.split(key, 7)
    feature_total = HEADS * DK
    fast_share = 0.5
    fast = jax.random.bernoulli(lookup_entries[0], fast_share, (feature_total,))
    fast_rate = jnp.exp(jax.random.uniform(lookup_entries[1], (feature_total,), jnp.float32, jnp.log(1.0 / 50.0), jnp.log(1.0 / 30.0)))
    slow_rate = jnp.exp(jax.random.uniform(lookup_entries[2], (feature_total,), jnp.float32, jnp.log(0.05), jnp.log(0.25))) / STREAM_LENGTH
    rate = jnp.where(fast, fast_rate, slow_rate)
    blocks = STREAM_LENGTH // TOK_DEV
    block_factor = jnp.exp(jax.random.uniform(lookup_entries[3], (blocks, 1, 1), jnp.float32, -0.7, 0.7))
    rough = jnp.exp(jax.random.uniform(lookup_entries[4], (blocks, TOK_DEV, feature_total), jnp.float32, -0.4, 0.4))
    stable_mode = -(rate[None, None, :] * block_factor * rough).reshape(STREAM_LENGTH, feature_total)
    spike_location = jax.random.randint(lookup_entries[5], (3,), 0, STREAM_LENGTH)
    spike_surcharge = jax.random.uniform(lookup_entries[6], (feature_total,), jnp.float32, 0.2, 0.5)
    spike_indicator = jnp.any(jnp.arange(STREAM_LENGTH)[:, None] == spike_location[None, :], axis=1)
    return stable_mode + jnp.where(spike_indicator[:, None], jnp.log(1.0 - spike_surcharge)[None, :], 0.0)


def strengthened(entries, rng, source, target, shards_of, factor):
    owner, partner = [(jnp.arange(entries.shape[dim]) // (entries.shape[dim] // shards_of)).reshape([-1 if axis == dim else 1 for axis in range(entries.ndim)]) for dim in (source, target)]
    chosen = jax.random.permutation(rng, shards_of)[partner]
    strong = (owner == chosen) | (owner == (partner + shards_of // 2) % shards_of)
    return jnp.where(strong, factor * entries, entries)


def steps_of(key, shape, shards, smallest, high):
    def one(axis_at, shards_of):
        draws = jax.random.uniform(jax.random.fold_in(jax.random.fold_in(key, 6), axis_at), (shards_of,), jnp.float32, smallest / len(shards), high / len(shards))
        return jnp.repeat(jnp.exp(draws), shape[axis_at] // shards_of).reshape((-1,) + (1,) * (len(shape) - axis_at - 1))

    level = one(*shards[0])
    for cut in shards[1:]:
        level = level * one(*cut)
    return level


def deal_out(rng, own, number, rows, amount, top, bound, slope):
    ranking = jax.random.permutation(rng, amount)
    packed, common = shares(amount, rows * top, bound, slope, True), shares(amount, rows * top, bound, slope, False)
    places = jnp.arange(amount)

    def named(lengths, turn):
        used = int((lengths > 0).sum())
        fixed = max(1, used // 4)
        shifted = fixed + (places - fixed + turn * (used - fixed)) % max(1, amount - fixed)
        return jnp.zeros((amount,), jnp.int32).at[ranking[jnp.where(places < fixed, places, shifted)]].set(jnp.asarray(lengths, jnp.int32))

    lengths = jnp.where(number % 4 == 0, named(packed, number // 4), named(common, number - number // 4 - 1))
    mixed = jax.random.permutation(jax.random.fold_in(own, 3), amount)
    source_of, receiver = mixed[0:amount // 2 * 2:2], mixed[1:amount // 2 * 2:2]
    margin = jnp.minimum(lengths[source_of] - 1, bound - lengths[receiver]) // 2
    margin = jnp.where((source_of == ranking[0]) | (receiver == ranking[0]) | (lengths[receiver] == 0), 0, jnp.maximum(margin, 0))
    shifted = jax.random.randint(jax.random.fold_in(own, 4), (amount // 2,), 0, 1 << 20) % (margin + 1)
    lengths = lengths.at[source_of].add(-shifted).at[receiver].add(shifted)
    labels = jnp.searchsorted(jnp.cumsum(lengths), jnp.arange(rows * top), side="right").astype(jnp.int32)
    listing = labels.reshape(top, rows).T
    listing = listing[jax.random.permutation(jax.random.fold_in(own, 1), rows)]
    turn = jax.random.randint(jax.random.fold_in(own, 2), (rows, 1), 0, top)
    return jnp.take_along_axis(listing, (jnp.arange(top)[None, :] + turn) % top, axis=1)


def shares(number_of, total, limit, skew, full):
    portions = [(1 << 20) // math.isqrt(grade ** skew) + 1 for grade in range(1, number_of + 1)]
    largest = limit if full else min(limit, max(-(-total // number_of), total * portions[0] // sum(portions)))
    least = 1 if total - largest >= number_of - 1 else 0
    holding, spare = [largest] + [least] * (number_of - 1), total - largest - least * (number_of - 1)
    while spare > 0:
        free = [i for i in range(1, number_of) if holding[i] < largest] or [i for i in range(1, number_of) if holding[i] < limit]
        whole, left = sum([portions[i] for i in free]), spare
        for i in free:
            more = min(limit - holding[i], max(1, left * portions[i] // whole), spare)
            holding[i] = holding[i] + more
            spare = spare - more
    return np.array(holding)


def normal_values(key, shape, spread, limit, shards=(), kind=jnp.bfloat16):
    loudness = steps_of(key, shape, shards, -0.22, 0.18) if shards else 1.0
    values = jax.random.normal(key, shape, jnp.float32) * spread * loudness
    return jnp.minimum(jnp.maximum(values, -limit), limit).astype(kind)


def noise_with(key, dims, scale, reach, shards, heavy, kind=jnp.bfloat16):
    result = scale * jax.random.normal(key, dims, jnp.float32)
    if shards:
        result = result * steps_of(key, dims, shards, -0.22, 0.18)
    return jnp.clip(strengthened(result, jax.random.fold_in(key, 3), *heavy), -reach, reach).astype(kind)


def setup_inputs(seed: int = 0) -> dict:
    splits = jax.random.split(jax.random.key(seed), 14)
    queries = normal_values(splits[0], (STREAM_LENGTH, HEADS * DK), 0.125, 0.75, ((0, 8), (1, 4)))
    key_vectors = normal_values(splits[1], (STREAM_LENGTH, HEADS * DK), 0.125, 0.75, ((0, 8), (1, 4)))
    values_in = normal_values(splits[2], (STREAM_LENGTH, HEADS * DV), 0.125, 0.75, ((0, 8), (1, 4)))
    log_decay = draw_log_decay(jax.random.fold_in(splits[13], 71), 0)
    mixed_heads = normal_values(splits[4], (STREAM_LENGTH, HEADS * DV), 1.0, 6.0, ((0, 8), (1, 4)))
    out_proj = normal_values(splits[5], (HEADS * DV, D), (HEADS * DV) ** -0.5, 0.125, ((0, 4),))
    layer_input = normal_values(splits[6], (STREAM_LENGTH, D), 1.0, 6.0, ((0, 8),))
    cotangent = noise_with(splits[7], (STREAM_LENGTH, D), 1.0, 6.0, ((0, 8),), (0, 1, 8, 2.0))
    routes_keys = jax.random.split(jax.random.fold_in(splits[8], 1), STREAM_LENGTH // TOK_DEV)
    routes_turns = jax.random.permutation(jax.random.fold_in(splits[8], 3), STREAM_LENGTH // TOK_DEV)
    routes = jax.vmap(lambda own, number: deal_out(jax.random.fold_in(splits[8], 2), own, number, TOK_DEV, EXPERTS, TOP, CAP, 2))(routes_keys, routes_turns).reshape((STREAM_LENGTH, TOP))
    route_weight = jnp.clip(jnp.exp(math.log(2.0) - 2.0794415 * jax.random.uniform(splits[9], (STREAM_LENGTH, TOP), jnp.float32) ** steps_of(splits[9], (STREAM_LENGTH, TOP), ((0, 8),), -0.2, 0.2)), 0.25, 2.0)
    gate_weight = normal_values(splits[10], (EXPERTS, D, FE), D ** -0.5, 0.125, ((0, 8), (2, 4)))
    up_weight = normal_values(splits[11], (EXPERTS, D, FE), D ** -0.5, 0.125, ((0, 8), (2, 4)))
    down_weight = normal_values(splits[12], (EXPERTS, FE, D), FE ** -0.5, 0.1875, ((0, 8), (1, 4)))
    return dict(queries=queries, key_vectors=key_vectors, values_in=values_in, log_decay=log_decay, mixed_heads=mixed_heads, out_proj=out_proj, layer_input=layer_input, cotangent=cotangent, routes=routes, route_weight=route_weight, gate_weight=gate_weight, up_weight=up_weight, down_weight=down_weight)


def local_parts(query_f, key_f, grad_f, pair, decays):
    highest = lax.Precision.HIGHEST
    sigma = query_f.shape[2] ** -0.5
    length = query_f.shape[0]
    cum = jnp.cumsum(decays, axis=0)
    total = cum[-1]
    middle = 0.5 * total
    rise = jnp.exp(cum - middle)
    fall = jnp.exp(middle - cum)
    position = jnp.arange(length, dtype=jnp.int32)
    lower = (position[:, None] >= position[None, :])[None]
    score_fwd = jnp.where(lower, jnp.einsum("thc,shc->hts", query_f * rise, key_f * fall, precision=highest), 0.0) * sigma
    score_bwd = jnp.where(lower, 0.0, jnp.einsum("thc,shc->hts", query_f * fall, key_f * rise, precision=highest)) * sigma
    pair_fwd = jnp.where(lower, pair, 0.0)
    pair_bwd = jnp.where(lower, 0.0, pair)
    query_fwd = sigma * rise * jnp.einsum("hts,shc->thc", pair_fwd, key_f * fall, precision=highest)
    query_bwd = sigma * fall * jnp.einsum("hts,shc->thc", pair_bwd, key_f * rise, precision=highest)
    key_fwd = sigma * fall * jnp.einsum("hts,thc->shc", pair_fwd, query_f * rise, precision=highest)
    key_bwd = sigma * rise * jnp.einsum("hts,thc->shc", pair_bwd, query_f * fall, precision=highest)
    value_grad = jnp.einsum("hts,thv->shv", score_fwd + score_bwd, grad_f, precision=highest)
    return query_fwd, query_bwd, key_fwd, key_bwd, value_grad, cum, total


def state_terms(query_f, key_f, value_f, grad_f, cum, total):
    highest = lax.Precision.HIGHEST
    head_part = jnp.exp(cum)
    tail = jnp.exp(total - cum)
    kv_fwd = jnp.einsum("shc,shv->hcv", key_f * tail, value_f, precision=highest)
    qo_bwd = jnp.einsum("thc,thv->hcv", query_f * tail, grad_f, precision=highest)
    qo_fwd = jnp.einsum("thc,thv->hcv", query_f * head_part, grad_f, precision=highest)
    kv_bwd = jnp.einsum("shc,shv->hcv", key_f * head_part, value_f, precision=highest)
    return jnp.exp(total), kv_fwd, qo_bwd, qo_fwd, kv_bwd


def carried(parts, states, query_f, key_f, value_f, grad_f):
    highest = lax.Precision.HIGHEST
    sigma = query_f.shape[2] ** -0.5
    query_fwd, query_bwd, key_fwd, key_bwd, value_grad, cum, total = parts
    kv_low, qo_low, qo_high, kv_high = states
    head_part = jnp.exp(cum)
    tail = jnp.exp(total - cum)
    query_fwd = query_fwd + sigma * head_part * jnp.einsum("thv,hcv->thc", grad_f, kv_low, precision=highest)
    query_bwd = query_bwd + sigma * tail * jnp.einsum("thv,hcv->thc", grad_f, kv_high, precision=highest)
    key_fwd = key_fwd + sigma * tail * jnp.einsum("shv,hcv->shc", value_f, qo_high, precision=highest)
    key_bwd = key_bwd + sigma * head_part * jnp.einsum("shv,hcv->shc", value_f, qo_low, precision=highest)
    value_grad = value_grad + sigma * (jnp.einsum("shc,hcv->shv", key_f * tail, qo_high, precision=highest)
                                       + jnp.einsum("shc,hcv->shv", key_f * head_part, qo_low, precision=highest))
    grad_cum = query_f * (query_fwd - query_bwd) - key_f * (key_fwd - key_bwd)
    return query_fwd + query_bwd, key_fwd + key_bwd, value_grad, grad_cum


def carry_step(carry, inputs):
    decay_all, first_term, second_term = inputs
    grown = (decay_all[..., None] * carry[0] + first_term, decay_all[..., None] * carry[1] + second_term)
    return grown, carry


def expert_grads(inputs):
    rows, cots, weights, gate_w, up_w, down_w = inputs
    pre_gate = jnp.dot(rows, gate_w, preferred_element_type=jnp.float32)
    pre_up = jnp.dot(rows, up_w, preferred_element_type=jnp.float32)
    weighted = (weights[:, None] * cots.astype(jnp.float32)).astype(jnp.bfloat16)
    d_act = jnp.dot(weighted, down_w.T, preferred_element_type=jnp.float32)
    sigmoid_gate = jax.nn.sigmoid(pre_gate)
    silu_gate = pre_gate * sigmoid_gate
    act = (silu_gate * pre_up).astype(jnp.bfloat16)
    d_gate = (d_act * pre_up * sigmoid_gate * (1.0 + pre_gate * (1.0 - sigmoid_gate))).astype(jnp.bfloat16)
    d_up = (d_act * silu_gate).astype(jnp.bfloat16)
    grad_down = jnp.dot(act.T, weighted, preferred_element_type=jnp.float32)
    grad_gate = jnp.dot(rows.T, d_gate, preferred_element_type=jnp.float32)
    grad_up = jnp.dot(rows.T, d_up, preferred_element_type=jnp.float32)
    part_width = FE // N_TP
    parts = jnp.einsum("rpf,pfd->rpd", d_gate.reshape(-1, N_TP, part_width).astype(jnp.float32),
                       gate_w.T.reshape(N_TP, part_width, D).astype(jnp.float32))
    parts = parts + jnp.einsum("rpf,pfd->rpd", d_up.reshape(-1, N_TP, part_width).astype(jnp.float32),
                               up_w.T.reshape(N_TP, part_width, D).astype(jnp.float32))
    rounded = lax.optimization_barrier(parts.astype(jnp.bfloat16))
    row_grad = jnp.sum(rounded.astype(jnp.float32), axis=1).astype(jnp.bfloat16)
    return grad_gate, grad_up, grad_down, row_grad


def reference(queries, key_vectors, values_in, log_decay, mixed_heads, out_proj, layer_input, cotangent,
              routes, route_weight, gate_weight, up_weight, down_weight):
    blocks = STREAM_LENGTH // TOK_DEV
    rows_all = blocks * CAP
    flat_route = routes.reshape(blocks, TOK_DEV * TOP)
    onehot = (flat_route[:, :, None] == jnp.arange(EXPERTS, dtype=jnp.int32)[None, None, :]).astype(jnp.int32)
    rank = jnp.sum((jnp.cumsum(onehot, axis=1) - onehot) * onehot, axis=2)
    block_id = jnp.arange(blocks, dtype=jnp.int32)[:, None]
    place = (flat_route * rows_all + block_id * CAP + rank).reshape(-1).astype(jnp.int32)
    token_id = jnp.arange(STREAM_LENGTH * TOP, dtype=jnp.int32) // TOP
    slot_token = jnp.zeros((EXPERTS * rows_all,), jnp.int32).at[place].set(token_id)
    filled = jnp.zeros((EXPERTS * rows_all,), jnp.float32).at[place].set(1.0)
    slot_weight = jnp.zeros((EXPERTS * rows_all,), jnp.float32).at[place].set(route_weight.reshape(-1))
    expert_rows = (layer_input[slot_token].astype(jnp.float32) * filled[:, None]).astype(jnp.bfloat16)
    expert_cot = (cotangent[slot_token].astype(jnp.float32) * filled[:, None]).astype(jnp.bfloat16)
    grad_gate, grad_up, grad_down, row_grad = lax.map(expert_grads, (
        expert_rows.reshape(EXPERTS, rows_all, D), expert_cot.reshape(EXPERTS, rows_all, D),
        slot_weight.reshape(EXPERTS, rows_all), gate_weight, up_weight, down_weight))
    back = row_grad.reshape(EXPERTS * rows_all, D)[place].reshape(STREAM_LENGTH, TOP, D)
    token_grad = (cotangent.astype(jnp.float32) + jnp.sum(back.astype(jnp.float32), axis=1)).astype(jnp.bfloat16)
    grad_proj = jnp.dot(token_grad.T, mixed_heads, preferred_element_type=jnp.float32)
    head_grad = jnp.dot(token_grad, out_proj.T, preferred_element_type=jnp.float32)

    highest = lax.Precision.HIGHEST
    query_f = queries.astype(jnp.float32).reshape(blocks, TOK_DEV, HEADS, DK)
    key_f = key_vectors.astype(jnp.float32).reshape(blocks, TOK_DEV, HEADS, DK)
    value_f = values_in.astype(jnp.float32).reshape(blocks, TOK_DEV, HEADS, DV)
    grad_f = head_grad.reshape(blocks, TOK_DEV, HEADS, DV)
    decays = log_decay.reshape(blocks, TOK_DEV, HEADS, DK)
    pair = jnp.einsum("bthv,bshv->bhts", grad_f, value_f, precision=highest)
    parts = jax.vmap(local_parts)(query_f, key_f, grad_f, pair, decays)
    terms = jax.vmap(state_terms)(query_f, key_f, value_f, grad_f, parts[5], parts[6])
    zeros = jnp.zeros((HEADS, DK, DV), jnp.float32)
    _, low = lax.scan(carry_step, (zeros, zeros), (terms[0], terms[1], terms[2]))
    _, high = lax.scan(carry_step, (zeros, zeros), (terms[0], terms[3], terms[4]), reverse=True)
    query_grad, key_grad, value_grad, grad_cum = jax.vmap(carried)(
        parts, (low[0], low[1], high[0], high[1]), query_f, key_f, value_f, grad_f)
    grad_cum = grad_cum.reshape(STREAM_LENGTH, HEADS * DK)
    grad_decay = jnp.flip(jnp.cumsum(jnp.flip(grad_cum, 0), axis=0), 0)
    return (grad_gate, grad_up, grad_down, grad_proj, query_grad.reshape(STREAM_LENGTH, HEADS * DK),
            key_grad.reshape(STREAM_LENGTH, HEADS * DK), value_grad.reshape(STREAM_LENGTH, HEADS * DV), grad_decay)
```

```python
import functools

import jax
import jax.numpy as jnp
from jax import lax
from jax.experimental import pallas as pl
from jax.experimental.pallas import tpu as pltpu
from jax.sharding import PartitionSpec as P

DK = 128
DV = 256
VMEM = pltpu.VMEM
ANY = pl.ANY


def remote(source, target, send_sem, recv_sem, device):
    return pltpu.make_async_remote_copy(
        src_ref=source,
        dst_ref=target,
        send_sem=send_sem,
        recv_sem=recv_sem,
        device_id=device,
        device_id_type=pl.DeviceIdType.MESH,
    )


def greet(seq, tensor, s, tp_peers):
    barrier = pltpu.get_barrier_semaphore()
    for d in range(1, seq):
        pl.semaphore_signal(
            barrier,
            inc=1,
            device_id={"sp": lax.rem(s + d, seq)},
            device_id_type=pl.DeviceIdType.MESH,
        )
    for peer in tp_peers:
        pl.semaphore_signal(
            barrier, inc=1, device_id={"tp": peer}, device_id_type=pl.DeviceIdType.MESH
        )
    pl.semaphore_wait(barrier, seq - 1 + len(tp_peers))


def neighbours(tensor):
    t = lax.axis_index("tp")
    beside = t + 1 - 2 * lax.rem(t, 2)
    across = lax.rem(t + tensor // 2, tensor)
    return t, beside, across


def dispatch_kernel(
    seq,
    tensor,
    width,
    rows_ref,
    cot_ref,
    total_ref,
    state_ref,
    rows_out,
    cot_out,
    total_out,
    state_out,
    sp_send,
    sp_recv,
    tp_send,
    tp_recv,
    small_send,
    small_recv,
    own_sem,
):
    s = lax.axis_index("sp")
    t, beside, across = neighbours(tensor)
    ins, outs = (rows_ref, cot_ref), (rows_out, cot_out)
    greet(seq, tensor, s, (beside, across))

    def place(a, block, part):
        return outs[a].at[:, block, :, pl.ds(pl.multiple_of(part * width, width), width)]

    def spread(a, d):
        to = lax.rem(s + d, seq)
        return remote(
            ins[a].at[to], place(a, s, t), sp_send.at[a, d], sp_recv.at[a, d], {"sp": to}
        )

    def origin(d):
        return lax.rem(s - d + seq, seq)

    def forward(a, d, way):
        block = origin(d)
        part = across if way == 2 else t
        source = ins[a].at[s] if d == 0 and way != 2 else place(a, block, part)
        return remote(
            source,
            place(a, block, part),
            tp_send.at[way, a, d],
            tp_recv.at[way, a, d],
            {"tp": across if way == 1 else beside},
        )

    def small(d, which):
        to = lax.rem(s + d, seq)
        if which == 0:
            source, target = total_ref, total_out.at[s]
        else:
            source, target = state_ref.at[jnp.where(to > s, 0, 1)], state_out.at[s]
        return remote(
            source, target, small_send.at[which, d], small_recv.at[which, d], {"sp": to}
        )

    for d in range(1, seq):
        for a in range(2):
            spread(a, d).start()
    own = [
        pltpu.make_async_copy(ins[a].at[s], place(a, s, t), own_sem.at[a]) for a in range(2)
    ] + [
        pltpu.make_async_copy(total_ref, total_out.at[s], own_sem.at[2]),
        pltpu.make_async_copy(state_ref.at[0], state_out.at[s], own_sem.at[3]),
    ]
    for copy in own:
        copy.start()
    for a in range(2):
        forward(a, 0, 1).start()
        forward(a, 0, 0).start()
    for d in range(1, seq):
        small(d, 0).start()
        small(d, 1).start()
    lag = 2
    for d in range(1, seq + lag):
        if d < seq:
            for a in range(2):
                spread(a, d).wait_recv()
                forward(a, d, 1).start()
                forward(a, d, 0).start()
        if d >= lag:
            for a in range(2):
                forward(a, d - lag, 1).wait_recv()
                forward(a, d - lag, 2).start()
    for d in range(seq):
        for a in range(2):
            if d:
                spread(a, d).wait_send()
            forward(a, d, 0).wait()
            forward(a, d, 1).wait_send()
            forward(a, d, 2).wait()
        if d:
            small(d, 0).wait()
            small(d, 1).wait()
    for copy in own:
        copy.wait()


def return_kernel(
    seq,
    tensor,
    width,
    part_ref,
    cot_ref,
    pick_ref,
    mixed_ref,
    token_out,
    mixed_out,
    arrived,
    summed,
    back,
    total,
    red_send,
    red_recv,
    sp_send,
    sp_recv,
    mix_send,
    mix_recv,
    tok_send,
    tok_recv,
    own_sem,
):
    s = lax.axis_index("sp")
    t, beside, across = neighbours(tensor)
    experts = part_ref.shape[0]
    greet(seq, tensor, s, tuple(lax.rem(t + u, tensor) for u in range(1, tensor)))

    def columns(part):
        return pl.ds(pl.multiple_of(part * width, width), width)

    def reduce(d, u):
        block = lax.rem(s + d, seq)
        to = lax.rem(t + u, tensor)
        return remote(
            part_ref.at[:, block, :, columns(to)],
            arrived.at[u - 1, d],
            red_send.at[u - 1, d],
            red_recv.at[u - 1, d],
            {"tp": to},
        )

    def give(d):
        to = lax.rem(s + d, seq)
        return remote(summed.at[d], back.at[d], sp_send.at[d], sp_recv.at[d], {"sp": to})

    def mix(d):
        to = lax.rem(s + d, seq)
        return remote(
            mixed_ref, mixed_out.at[s], mix_send.at[d], mix_recv.at[d], {"sp": to}
        )

    def token(way):
        part = across if way == 2 else t
        return remote(
            token_out.at[part],
            token_out.at[part],
            tok_send.at[way],
            tok_recv.at[way],
            {"tp": across if way == 1 else beside},
        )

    order = list(range(1, seq)) + [0]
    for d in order:
        for u in range(1, tensor):
            reduce(d, u).start()
    own = pltpu.make_async_copy(mixed_ref, mixed_out.at[s], own_sem)
    own.start()
    for d in range(1, seq):
        mix(d).start()
    for d in order:
        block = lax.rem(s + d, seq)
        for u in range(1, tensor):
            reduce(d, u).wait_recv()
        for e in range(experts):
            value = part_ref[e, block, :, columns(t)].astype(jnp.float32)
            for u in range(1, tensor):
                value += arrived[u - 1, d, e].astype(jnp.float32)
            summed[d, e] = value.astype(jnp.bfloat16)
        if d:
            give(d).start()
    total[...] = cot_ref[...].astype(jnp.float32)
    for d in [0] + list(range(1, seq)):
        block = lax.rem(s - d + seq, seq)
        if d:
            give(d).wait_recv()
        held = back if d else summed
        term = total[...]
        for e in range(experts):
            term += jnp.dot(
                pick_ref[block, e], held[d, e], preferred_element_type=jnp.float32
            )
        total[...] = term
    token_out[t] = total[...].astype(jnp.bfloat16)
    token(1).start()
    token(0).start()
    token(1).wait_recv()
    token(2).start()
    for d in range(seq):
        for u in range(1, tensor):
            reduce(d, u).wait_send()
        if d:
            give(d).wait_send()
            mix(d).wait()
    own.wait()
    token(0).wait()
    token(1).wait_send()
    token(2).wait()


def exchange_kernel(
    seq, tensor, state_ref, token_ref, state_out, token_out, send_sem, recv_sem, own_sem
):
    s = lax.axis_index("sp")
    greet(seq, tensor, s, ())

    def copy(d, which):
        to = lax.rem(s + d, seq)
        if which == 0:
            source, target = state_ref.at[jnp.where(to > s, 0, 1)], state_out.at[s]
        else:
            source, target = token_ref.at[to], token_out.at[s]
        return remote(source, target, send_sem.at[which, d], recv_sem.at[which, d], {"sp": to})

    own = (
        pltpu.make_async_copy(state_ref.at[0], state_out.at[s], own_sem.at[0]),
        pltpu.make_async_copy(token_ref.at[s], token_out.at[s], own_sem.at[1]),
    )
    for which in range(2):
        for d in range(1, seq):
            copy(d, which).start()
    for piece in own:
        piece.start()
    for which in range(2):
        for d in range(1, seq):
            copy(d, which).wait()
    for piece in own:
        piece.wait()


def call(kernel, outs, in_spaces, out_spaces, scratch, number):
    return pl.pallas_call(
        kernel,
        out_shape=outs,
        in_specs=[pl.BlockSpec(memory_space=space) for space in in_spaces],
        out_specs=[pl.BlockSpec(memory_space=space) for space in out_spaces],
        scratch_shapes=scratch,
        compiler_params=pltpu.CompilerParams(collective_id=number, has_side_effects=True),
    )


def running_sum(value):
    row = jnp.arange(value.shape[0], dtype=jnp.int32)
    mask = (row[:, None] >= row[None, :]).astype(jnp.float32)
    return jnp.tensordot(mask, value, 1, precision=lax.Precision.HIGHEST)


def tail_sum(value):
    row = jnp.arange(value.shape[0], dtype=jnp.int32)
    mask = (row[:, None] <= row[None, :]).astype(jnp.float32)
    return jnp.tensordot(mask, value, 1, precision=lax.Precision.HIGHEST)


def local_parts(query_f, key_f, grad_f, pair, decays):
    highest = lax.Precision.HIGH
    sigma = query_f.shape[2] ** (-0.5)
    length = query_f.shape[0]
    cum = running_sum(decays)
    total = cum[-1]
    middle = 0.5 * total
    rise = jnp.exp(cum - middle)
    fall = jnp.exp(middle - cum)
    position = jnp.arange(length, dtype=jnp.int32)
    lower = (position[:, None] >= position[None, :])[None]
    score_fwd = (
        jnp.where(
            lower, jnp.einsum("thc,shc->hts", query_f * rise, key_f * fall, precision=highest), 0.0
        )
        * sigma
    )
    score_bwd = (
        jnp.where(
            lower, 0.0, jnp.einsum("thc,shc->hts", query_f * fall, key_f * rise, precision=highest)
        )
        * sigma
    )
    pair_fwd = jnp.where(lower, pair, 0.0)
    pair_bwd = jnp.where(lower, 0.0, pair)
    query_fwd = sigma * rise * jnp.einsum("hts,shc->thc", pair_fwd, key_f * fall, precision=highest)
    query_bwd = sigma * fall * jnp.einsum("hts,shc->thc", pair_bwd, key_f * rise, precision=highest)
    key_fwd = sigma * fall * jnp.einsum("hts,thc->shc", pair_fwd, query_f * rise, precision=highest)
    key_bwd = sigma * rise * jnp.einsum("hts,thc->shc", pair_bwd, query_f * fall, precision=highest)
    value_grad = jnp.einsum("hts,thv->shv", score_fwd + score_bwd, grad_f, precision=highest)
    return (query_fwd, query_bwd, key_fwd, key_bwd, value_grad, cum, total)


def state_terms(query_f, key_f, value_f, grad_f, cum, total):
    highest = lax.Precision.HIGH
    head_part = jnp.exp(cum)
    tail = jnp.exp(total - cum)
    kv_fwd = jnp.einsum("shc,shv->hcv", key_f * tail, value_f, precision=highest)
    qo_bwd = jnp.einsum("thc,thv->hcv", query_f * tail, grad_f, precision=highest)
    qo_fwd = jnp.einsum("thc,thv->hcv", query_f * head_part, grad_f, precision=highest)
    kv_bwd = jnp.einsum("shc,shv->hcv", key_f * head_part, value_f, precision=highest)
    return (jnp.exp(total), kv_fwd, qo_bwd, qo_fwd, kv_bwd)


def carried(parts, states, query_f, key_f, value_f, grad_f):
    highest = lax.Precision.HIGH
    sigma = query_f.shape[2] ** (-0.5)
    query_fwd, query_bwd, key_fwd, key_bwd, value_grad, cum, total = parts
    kv_low, qo_low, qo_high, kv_high = states
    head_part = jnp.exp(cum)
    tail = jnp.exp(total - cum)
    query_fwd = query_fwd + sigma * head_part * jnp.einsum(
        "thv,hcv->thc", grad_f, kv_low, precision=highest
    )
    query_bwd = query_bwd + sigma * tail * jnp.einsum(
        "thv,hcv->thc", grad_f, kv_high, precision=highest
    )
    key_fwd = key_fwd + sigma * tail * jnp.einsum(
        "shv,hcv->shc", value_f, qo_high, precision=highest
    )
    key_bwd = key_bwd + sigma * head_part * jnp.einsum(
        "shv,hcv->shc", value_f, qo_low, precision=highest
    )
    value_grad = value_grad + sigma * (
        jnp.einsum("shc,hcv->shv", key_f * tail, qo_high, precision=highest)
        + jnp.einsum("shc,hcv->shv", key_f * head_part, qo_low, precision=highest)
    )
    grad_cum = query_f * (query_fwd - query_bwd) - key_f * (key_fwd - key_bwd)
    return (query_fwd + query_bwd, key_fwd + key_bwd, value_grad, grad_cum)


def body(
    queries,
    key_vectors,
    values_in,
    log_decay,
    mixed_heads,
    out_proj,
    layer_input,
    cotangent,
    routes,
    route_weight,
    gate_weight,
    up_weight,
    down_weight,
):
    tokens, top = routes.shape
    seq = lax.axis_size("sp")
    tensor = lax.axis_size("tp")
    s = lax.axis_index("sp")
    experts = gate_weight.shape[0]
    all_experts = experts * seq
    capacity = 2 * tokens * top // all_experts
    model = cotangent.shape[1]
    width = model // tensor
    column = lax.axis_index("tp") * width
    bf16, f32 = jnp.bfloat16, jnp.float32
    dma = pltpu.SemaphoreType.DMA

    heads = queries.shape[1] // DK
    query_f = queries.reshape(tokens, heads, DK).astype(f32)
    key_f = key_vectors.reshape(tokens, heads, DK).astype(f32)
    value_f = values_in.reshape(tokens, heads, DV).astype(f32)
    decays = log_decay.reshape(tokens, heads, DK)
    cum = running_sum(decays)
    total = cum[-1]
    head_part = jnp.exp(cum)
    tail = jnp.exp(total - cum)
    high = lax.Precision.HIGH
    kv_fwd = jnp.einsum("shc,shv->hcv", key_f * tail, value_f, precision=high)
    kv_bwd = jnp.einsum("shc,shv->hcv", key_f * head_part, value_f, precision=high)
    kv_send = jnp.stack([kv_fwd, kv_bwd]).astype(bf16)

    flat_route = routes.reshape(-1)
    onehot = flat_route[:, None] == jnp.arange(all_experts, dtype=jnp.int32)[None, :]
    pair_id = jnp.arange(tokens * top, dtype=jnp.int32)
    before = (pair_id[:, None] > pair_id[None, :]).astype(bf16)
    counts = jnp.dot(before, onehot.astype(bf16), preferred_element_type=f32)
    rank = jnp.sum(jnp.where(onehot, counts, 0.0), axis=1).astype(jnp.int32)
    slot = (flat_route * capacity + rank).reshape(tokens, top)
    slot_id = jnp.arange(all_experts * capacity, dtype=jnp.int32)
    match = slot_id[:, None, None] == slot[None, :, :]
    chosen = jnp.any(match, axis=2).astype(bf16)
    slot_weight = jnp.sum(jnp.where(match, route_weight[None], 0.0), axis=(1, 2))
    pick = (
        jnp.any(
            slot_id.reshape(seq, experts, 1, capacity, 1) == slot[None, None, :, None, :], axis=4
        )
    ).astype(bf16)
    own_input = lax.dynamic_slice_in_dim(layer_input, column, width, 1)
    own_cot = lax.dynamic_slice_in_dim(cotangent, column, width, 1)
    block_shape = (seq, experts, capacity, width)
    rows_send = jnp.dot(chosen, own_input, preferred_element_type=f32).astype(bf16)
    cot_send = (
        slot_weight[:, None] * jnp.dot(chosen, own_cot, preferred_element_type=f32)
    ).astype(bf16)

    expert_shape = jax.ShapeDtypeStruct((experts, seq, capacity, model), bf16)
    expert_rows, weighted, total_all, kv_all = call(
        functools.partial(dispatch_kernel, seq, tensor, width),
        (
            expert_shape,
            expert_shape,
            jax.ShapeDtypeStruct((seq, heads, DK), f32),
            jax.ShapeDtypeStruct((seq, heads, DK, DV), bf16),
        ),
        (VMEM, VMEM, VMEM, VMEM),
        (ANY, ANY, VMEM, VMEM),
        [
            dma((2, seq)),
            dma((2, seq)),
            dma((3, 2, seq)),
            dma((3, 2, seq)),
            dma((2, seq)),
            dma((2, seq)),
            dma((4,)),
        ],
        0,
    )(rows_send.reshape(block_shape), cot_send.reshape(block_shape), total, kv_send)
    expert_rows = expert_rows.reshape(experts, seq * capacity, model)
    weighted = weighted.reshape(experts, seq * capacity, model)

    pre_gate = jnp.einsum("erd,edf->erf", expert_rows, gate_weight, preferred_element_type=f32)
    pre_up = jnp.einsum("erd,edf->erf", expert_rows, up_weight, preferred_element_type=f32)
    d_act = jnp.einsum("erd,efd->erf", weighted, down_weight, preferred_element_type=f32)
    sigmoid_gate = jax.nn.sigmoid(pre_gate)
    silu_gate = pre_gate * sigmoid_gate
    act = (silu_gate * pre_up).astype(bf16)
    d_gate = (d_act * pre_up * sigmoid_gate * (1.0 + pre_gate * (1.0 - sigmoid_gate))).astype(bf16)
    d_up = (d_act * silu_gate).astype(bf16)
    partial_value = (
        jnp.einsum("erf,edf->erd", d_gate, gate_weight, preferred_element_type=f32)
        + jnp.einsum("erf,edf->erd", d_up, up_weight, preferred_element_type=f32)
    ).astype(bf16)
    grad_gate, grad_up, grad_down = (
        jnp.einsum("erd,erf->edf", expert_rows, d_gate, preferred_element_type=f32),
        jnp.einsum("erd,erf->edf", expert_rows, d_up, preferred_element_type=f32),
        jnp.einsum("erf,erd->efd", act, weighted, preferred_element_type=f32),
    )

    token_parts, mixed_all = call(
        functools.partial(return_kernel, seq, tensor, width),
        (
            jax.ShapeDtypeStruct((tensor, tokens, width), bf16),
            jax.ShapeDtypeStruct((seq,) + mixed_heads.shape, bf16),
        ),
        (VMEM, VMEM, VMEM, VMEM),
        (VMEM, ANY),
        [
            pltpu.VMEM((tensor - 1,) + block_shape, bf16),
            pltpu.VMEM(block_shape, bf16),
            pltpu.VMEM(block_shape, bf16),
            pltpu.VMEM((tokens, width), f32),
            dma((tensor - 1, seq)),
            dma((tensor - 1, seq)),
            dma((seq,)),
            dma((seq,)),
            dma((seq,)),
            dma((seq,)),
            dma((3,)),
            dma((3,)),
            dma,
        ],
        1,
    )(
        partial_value.reshape(experts, seq, capacity, model),
        own_cot,
        pick,
        mixed_heads,
    )
    token_grad = jnp.transpose(token_parts, (1, 0, 2)).reshape(tokens, model)
    head_grad = lax.dot_general(
        token_grad, out_proj, (((1,), (1,)), ((), ())), preferred_element_type=f32
    )
    grad_f = head_grad.reshape(tokens, heads, DV)
    qo_bwd = jnp.einsum("thc,thv->hcv", query_f * tail, grad_f, precision=high)
    qo_fwd = jnp.einsum("thc,thv->hcv", query_f * head_part, grad_f, precision=high)
    qo_send = jnp.stack([qo_bwd, qo_fwd]).astype(bf16)
    share = model // seq
    token_send = jnp.transpose(token_grad.reshape(tokens, seq, share), (1, 0, 2))
    qo_all, token_all = call(
        functools.partial(exchange_kernel, seq, tensor),
        (
            jax.ShapeDtypeStruct((seq, heads, DK, DV), bf16),
            jax.ShapeDtypeStruct((seq, tokens, share), bf16),
        ),
        (VMEM, VMEM),
        (VMEM, VMEM),
        [dma((2, seq)), dma((2, seq)), dma((2,))],
        2,
    )(qo_send, token_send)
    grad_proj = lax.dot_general(
        token_all, mixed_all, (((0, 1), (0, 1)), ((), ())), preferred_element_type=f32
    )

    pair = jnp.einsum("thv,shv->hts", grad_f, value_f, precision=high)
    parts = local_parts(query_f, key_f, grad_f, pair, decays)
    block = jnp.arange(seq, dtype=jnp.int32)
    low_span = ((block[None, :] > block[:, None]) & (block[None, :] < s)).astype(f32)
    high_span = ((block[None, :] < block[:, None]) & (block[None, :] > s)).astype(f32)

    def carry(span, mask):
        logs = jnp.sum(span[:, :, None, None] * total_all[None], axis=1)
        return jnp.where(mask[:, None, None], jnp.exp(logs), 0.0)[..., None]

    low_scale = carry(low_span, block < s)
    high_scale = carry(high_span, block > s)
    kv_low = jnp.sum(low_scale * kv_all.astype(f32), axis=0)
    kv_high = jnp.sum(high_scale * kv_all.astype(f32), axis=0)
    qo_low = jnp.sum(low_scale * qo_all.astype(f32), axis=0)
    qo_high = jnp.sum(high_scale * qo_all.astype(f32), axis=0)
    query_grad, key_grad, value_grad, grad_cum = carried(
        parts, (kv_low, qo_low, qo_high, kv_high), query_f, key_f, value_f, grad_f
    )
    decay_all = jnp.exp(total)[..., None]
    beyond = DK ** (-0.5) * jnp.sum(
        (decay_all * kv_low + kv_fwd) * qo_high + (decay_all * qo_low + qo_bwd) * kv_high, axis=2
    )
    grad_decay = tail_sum(grad_cum) + beyond[None]
    return (
        grad_gate,
        grad_up,
        grad_down,
        grad_proj,
        query_grad.reshape(tokens, heads * DK),
        key_grad.reshape(tokens, heads * DK),
        value_grad.reshape(tokens, heads * DV),
        grad_decay.reshape(tokens, heads * DK),
    )


def solution(mesh):
    return jax.shard_map(
        body,
        mesh=mesh,
        in_specs=(
            P("sp", "tp"),
            P("sp", "tp"),
            P("sp", "tp"),
            P("sp", "tp"),
            P("sp", "tp"),
            P("tp", None),
            P("sp", None),
            P("sp", None),
            P("sp", None),
            P("sp", None),
            P("sp", None, "tp"),
            P("sp", None, "tp"),
            P("sp", "tp", None),
        ),
        out_specs=(
            P("sp", None, "tp"),
            P("sp", None, "tp"),
            P("sp", "tp", None),
            P("sp", "tp"),
            P("sp", "tp"),
            P("sp", "tp"),
            P("sp", "tp"),
            P("sp", "tp"),
        ),
        check_vma=False,
    )
```

```python
import functools

import jax
import jax.numpy as jnp
from jax import lax
from jax.experimental import pallas as pl
from jax.experimental.pallas import tpu as pltpu
from jax.sharding import PartitionSpec as P

DK = 128
DV = 256
VMEM = pltpu.VMEM
ANY = pl.ANY


def remote(source, target, send_sem, recv_sem, device):
    return pltpu.make_async_remote_copy(
        src_ref=source,
        dst_ref=target,
        send_sem=send_sem,
        recv_sem=recv_sem,
        device_id=device,
        device_id_type=pl.DeviceIdType.MESH,
    )


def greet(seq, tensor, s, tp_peers):
    barrier = pltpu.get_barrier_semaphore()
    for d in range(1, seq):
        pl.semaphore_signal(
            barrier,
            inc=1,
            device_id={"sp": lax.rem(s + d, seq)},
            device_id_type=pl.DeviceIdType.MESH,
        )
    for peer in tp_peers:
        pl.semaphore_signal(
            barrier, inc=1, device_id={"tp": peer}, device_id_type=pl.DeviceIdType.MESH
        )
    pl.semaphore_wait(barrier, seq - 1 + len(tp_peers))


def neighbours(tensor):
    t = lax.axis_index("tp")
    beside = t + 1 - 2 * lax.rem(t, 2)
    across = lax.rem(t + tensor // 2, tensor)
    return t, beside, across


class Relay:
    def __init__(self, seq, s, source, out, send_sem, recv_sem):
        self.half = seq // 2
        other = s + 1 - 2 * lax.rem(s, 2)

        def direct(j):
            to = lax.rem(s + 2 * j, seq)
            return remote(source(to), out.at[s], send_sem(j), recv_sem(j), {"sp": to})

        def onward(j):
            block = lax.rem(s - 2 * j + seq, seq)
            place = self.half + j
            held = out.at[block] if j else source(other)
            return remote(held, out.at[block], send_sem(place), recv_sem(place), {"sp": other})

        self.direct, self.onward = direct, onward

    def start(self):
        for j in range(1, self.half):
            self.direct(j).start()
        self.onward(0).start()

    def forward(self):
        for j in range(1, self.half):
            self.direct(j).wait_recv()
            self.onward(j).start()

    def finish(self):
        for j in range(self.half):
            if j:
                self.direct(j).wait_send()
            self.onward(j).wait()


def dispatch_kernel(
    seq,
    tensor,
    width,
    rows_ref,
    cot_ref,
    total_ref,
    state_ref,
    rows_out,
    cot_out,
    total_out,
    state_out,
    sp_send,
    sp_recv,
    tp_send,
    tp_recv,
    small_send,
    small_recv,
    own_sem,
):
    s = lax.axis_index("sp")
    t, beside, across = neighbours(tensor)
    ins, outs = (rows_ref, cot_ref), (rows_out, cot_out)
    greet(seq, tensor, s, (beside, across))

    def place(a, block, part):
        return outs[a].at[:, block, :, pl.ds(pl.multiple_of(part * width, width), width)]

    def spread(a, d):
        to = lax.rem(s + d, seq)
        return remote(
            ins[a].at[to], place(a, s, t), sp_send.at[a, d], sp_recv.at[a, d], {"sp": to}
        )

    def origin(d):
        return lax.rem(s - d + seq, seq)

    def forward(a, d, way):
        block = origin(d)
        part = across if way == 2 else t
        source = ins[a].at[s] if d == 0 and way != 2 else place(a, block, part)
        return remote(
            source,
            place(a, block, part),
            tp_send.at[way, a, d],
            tp_recv.at[way, a, d],
            {"tp": across if way == 1 else beside},
        )

    def small(d):
        to = lax.rem(s + d, seq)
        return remote(
            total_ref, total_out.at[s], small_send.at[0, d], small_recv.at[0, d], {"sp": to}
        )

    states = Relay(
        seq,
        s,
        lambda to: state_ref.at[jnp.where(to > s, 0, 1)],
        state_out,
        lambda i: small_send.at[1, i],
        lambda i: small_recv.at[1, i],
    )

    for d in range(1, seq):
        for a in range(2):
            spread(a, d).start()
    own = [
        pltpu.make_async_copy(ins[a].at[s], place(a, s, t), own_sem.at[a]) for a in range(2)
    ] + [
        pltpu.make_async_copy(total_ref, total_out.at[s], own_sem.at[2]),
        pltpu.make_async_copy(state_ref.at[0], state_out.at[s], own_sem.at[3]),
    ]
    for copy in own:
        copy.start()
    for a in range(2):
        forward(a, 0, 1).start()
        forward(a, 0, 0).start()
    for d in range(1, seq):
        small(d).start()
    states.start()
    lag = 2
    for d in range(1, seq + lag):
        if d < seq:
            for a in range(2):
                spread(a, d).wait_recv()
                forward(a, d, 1).start()
                forward(a, d, 0).start()
        if d >= lag:
            for a in range(2):
                forward(a, d - lag, 1).wait_recv()
                forward(a, d - lag, 2).start()
    states.forward()
    for d in range(seq):
        for a in range(2):
            if d:
                spread(a, d).wait_send()
            forward(a, d, 0).wait()
            forward(a, d, 1).wait_send()
            forward(a, d, 2).wait()
        if d:
            small(d).wait()
    states.finish()
    for copy in own:
        copy.wait()


def return_kernel(
    seq,
    tensor,
    width,
    part_ref,
    cot_ref,
    pick_ref,
    mixed_ref,
    token_out,
    mixed_out,
    arrived,
    summed,
    back,
    total,
    red_send,
    red_recv,
    sp_send,
    sp_recv,
    mix_send,
    mix_recv,
    tok_send,
    tok_recv,
    own_sem,
):
    s = lax.axis_index("sp")
    t, beside, across = neighbours(tensor)
    experts = part_ref.shape[0]
    greet(seq, tensor, s, tuple(lax.rem(t + u, tensor) for u in range(1, tensor)))

    def columns(part):
        return pl.ds(pl.multiple_of(part * width, width), width)

    def reduce(d, u):
        block = lax.rem(s + d, seq)
        to = lax.rem(t + u, tensor)
        return remote(
            part_ref.at[:, block, :, columns(to)],
            arrived.at[u - 1, d],
            red_send.at[u - 1, d],
            red_recv.at[u - 1, d],
            {"tp": to},
        )

    def give(d):
        to = lax.rem(s + d, seq)
        return remote(summed.at[d], back.at[d], sp_send.at[d], sp_recv.at[d], {"sp": to})

    mix = Relay(
        seq,
        s,
        lambda to: mixed_ref,
        mixed_out,
        lambda i: mix_send.at[i],
        lambda i: mix_recv.at[i],
    )

    def token(way):
        part = across if way == 2 else t
        return remote(
            token_out.at[part],
            token_out.at[part],
            tok_send.at[way],
            tok_recv.at[way],
            {"tp": across if way == 1 else beside},
        )

    order = list(range(1, seq)) + [0]
    for d in order:
        for u in range(1, tensor):
            reduce(d, u).start()
    own = pltpu.make_async_copy(mixed_ref, mixed_out.at[s], own_sem)
    own.start()
    mix.start()
    for d in order:
        block = lax.rem(s + d, seq)
        for u in range(1, tensor):
            reduce(d, u).wait_recv()
        for e in range(experts):
            value = part_ref[e, block, :, columns(t)].astype(jnp.float32)
            for u in range(1, tensor):
                value += arrived[u - 1, d, e].astype(jnp.float32)
            summed[d, e] = value.astype(jnp.bfloat16)
        if d:
            give(d).start()
    mix.forward()
    total[...] = cot_ref[...].astype(jnp.float32)
    for d in [0] + list(range(1, seq)):
        block = lax.rem(s - d + seq, seq)
        if d:
            give(d).wait_recv()
        held = back if d else summed
        term = total[...]
        for e in range(experts):
            term += jnp.dot(
                pick_ref[block, e], held[d, e], preferred_element_type=jnp.float32
            )
        total[...] = term
    token_out[t] = total[...].astype(jnp.bfloat16)
    token(1).start()
    token(0).start()
    token(1).wait_recv()
    token(2).start()
    for d in range(seq):
        for u in range(1, tensor):
            reduce(d, u).wait_send()
        if d:
            give(d).wait_send()
    mix.finish()
    own.wait()
    token(0).wait()
    token(1).wait_send()
    token(2).wait()


def exchange_kernel(
    seq, tensor, state_ref, token_ref, state_out, token_out, send_sem, recv_sem, own_sem
):
    s = lax.axis_index("sp")
    greet(seq, tensor, s, ())

    states = Relay(
        seq,
        s,
        lambda to: state_ref.at[jnp.where(to > s, 0, 1)],
        state_out,
        lambda i: send_sem.at[0, i],
        lambda i: recv_sem.at[0, i],
    )

    def copy(d):
        to = lax.rem(s + d, seq)
        return remote(
            token_ref.at[to], token_out.at[s], send_sem.at[1, d], recv_sem.at[1, d], {"sp": to}
        )

    own = (
        pltpu.make_async_copy(state_ref.at[0], state_out.at[s], own_sem.at[0]),
        pltpu.make_async_copy(token_ref.at[s], token_out.at[s], own_sem.at[1]),
    )
    states.start()
    for d in range(1, seq):
        copy(d).start()
    for piece in own:
        piece.start()
    states.forward()
    for d in range(1, seq):
        copy(d).wait()
    states.finish()
    for piece in own:
        piece.wait()


def call(kernel, outs, in_spaces, out_spaces, scratch, number):
    return pl.pallas_call(
        kernel,
        out_shape=outs,
        in_specs=[pl.BlockSpec(memory_space=space) for space in in_spaces],
        out_specs=[pl.BlockSpec(memory_space=space) for space in out_spaces],
        scratch_shapes=scratch,
        compiler_params=pltpu.CompilerParams(collective_id=number, has_side_effects=True),
    )


def running_sum(value):
    row = jnp.arange(value.shape[0], dtype=jnp.int32)
    mask = (row[:, None] >= row[None, :]).astype(jnp.float32)
    return jnp.tensordot(mask, value, 1, precision=lax.Precision.HIGHEST)


def tail_sum(value):
    row = jnp.arange(value.shape[0], dtype=jnp.int32)
    mask = (row[:, None] <= row[None, :]).astype(jnp.float32)
    return jnp.tensordot(mask, value, 1, precision=lax.Precision.HIGHEST)


def local_parts(query_f, key_f, grad_f, pair, decays):
    highest = lax.Precision.HIGH
    sigma = query_f.shape[2] ** (-0.5)
    length = query_f.shape[0]
    cum = running_sum(decays)
    total = cum[-1]
    middle = 0.5 * total
    rise = jnp.exp(cum - middle)
    fall = jnp.exp(middle - cum)
    position = jnp.arange(length, dtype=jnp.int32)
    lower = (position[:, None] >= position[None, :])[None]
    score_fwd = (
        jnp.where(
            lower, jnp.einsum("thc,shc->hts", query_f * rise, key_f * fall, precision=highest), 0.0
        )
        * sigma
    )
    score_bwd = (
        jnp.where(
            lower, 0.0, jnp.einsum("thc,shc->hts", query_f * fall, key_f * rise, precision=highest)
        )
        * sigma
    )
    pair_fwd = jnp.where(lower, pair, 0.0)
    pair_bwd = jnp.where(lower, 0.0, pair)
    query_fwd = sigma * rise * jnp.einsum("hts,shc->thc", pair_fwd, key_f * fall, precision=highest)
    query_bwd = sigma * fall * jnp.einsum("hts,shc->thc", pair_bwd, key_f * rise, precision=highest)
    key_fwd = sigma * fall * jnp.einsum("hts,thc->shc", pair_fwd, query_f * rise, precision=highest)
    key_bwd = sigma * rise * jnp.einsum("hts,thc->shc", pair_bwd, query_f * fall, precision=highest)
    value_grad = jnp.einsum("hts,thv->shv", score_fwd + score_bwd, grad_f, precision=highest)
    return (query_fwd, query_bwd, key_fwd, key_bwd, value_grad, cum, total)


def state_terms(query_f, key_f, value_f, grad_f, cum, total):
    highest = lax.Precision.HIGH
    head_part = jnp.exp(cum)
    tail = jnp.exp(total - cum)
    kv_fwd = jnp.einsum("shc,shv->hcv", key_f * tail, value_f, precision=highest)
    qo_bwd = jnp.einsum("thc,thv->hcv", query_f * tail, grad_f, precision=highest)
    qo_fwd = jnp.einsum("thc,thv->hcv", query_f * head_part, grad_f, precision=highest)
    kv_bwd = jnp.einsum("shc,shv->hcv", key_f * head_part, value_f, precision=highest)
    return (jnp.exp(total), kv_fwd, qo_bwd, qo_fwd, kv_bwd)


def carried(parts, states, query_f, key_f, value_f, grad_f):
    highest = lax.Precision.HIGH
    sigma = query_f.shape[2] ** (-0.5)
    query_fwd, query_bwd, key_fwd, key_bwd, value_grad, cum, total = parts
    kv_low, qo_low, qo_high, kv_high = states
    head_part = jnp.exp(cum)
    tail = jnp.exp(total - cum)
    query_fwd = query_fwd + sigma * head_part * jnp.einsum(
        "thv,hcv->thc", grad_f, kv_low, precision=highest
    )
    query_bwd = query_bwd + sigma * tail * jnp.einsum(
        "thv,hcv->thc", grad_f, kv_high, precision=highest
    )
    key_fwd = key_fwd + sigma * tail * jnp.einsum(
        "shv,hcv->shc", value_f, qo_high, precision=highest
    )
    key_bwd = key_bwd + sigma * head_part * jnp.einsum(
        "shv,hcv->shc", value_f, qo_low, precision=highest
    )
    value_grad = value_grad + sigma * (
        jnp.einsum("shc,hcv->shv", key_f * tail, qo_high, precision=highest)
        + jnp.einsum("shc,hcv->shv", key_f * head_part, qo_low, precision=highest)
    )
    grad_cum = query_f * (query_fwd - query_bwd) - key_f * (key_fwd - key_bwd)
    return (query_fwd + query_bwd, key_fwd + key_bwd, value_grad, grad_cum)


def body(
    queries,
    key_vectors,
    values_in,
    log_decay,
    mixed_heads,
    out_proj,
    layer_input,
    cotangent,
    routes,
    route_weight,
    gate_weight,
    up_weight,
    down_weight,
):
    tokens, top = routes.shape
    seq = lax.axis_size("sp")
    tensor = lax.axis_size("tp")
    s = lax.axis_index("sp")
    experts = gate_weight.shape[0]
    all_experts = experts * seq
    capacity = 2 * tokens * top // all_experts
    model = cotangent.shape[1]
    width = model // tensor
    column = lax.axis_index("tp") * width
    bf16, f32 = jnp.bfloat16, jnp.float32
    dma = pltpu.SemaphoreType.DMA

    heads = queries.shape[1] // DK
    query_f = queries.reshape(tokens, heads, DK).astype(f32)
    key_f = key_vectors.reshape(tokens, heads, DK).astype(f32)
    value_f = values_in.reshape(tokens, heads, DV).astype(f32)
    decays = log_decay.reshape(tokens, heads, DK)
    cum = running_sum(decays)
    total = cum[-1]
    head_part = jnp.exp(cum)
    tail = jnp.exp(total - cum)
    high = lax.Precision.HIGH
    kv_fwd = jnp.einsum("shc,shv->hcv", key_f * tail, value_f, precision=high)
    kv_bwd = jnp.einsum("shc,shv->hcv", key_f * head_part, value_f, precision=high)
    kv_send = jnp.stack([kv_fwd, kv_bwd]).astype(bf16)

    flat_route = routes.reshape(-1)
    onehot = flat_route[:, None] == jnp.arange(all_experts, dtype=jnp.int32)[None, :]
    pair_id = jnp.arange(tokens * top, dtype=jnp.int32)
    before = (pair_id[:, None] > pair_id[None, :]).astype(bf16)
    counts = jnp.dot(before, onehot.astype(bf16), preferred_element_type=f32)
    rank = jnp.sum(jnp.where(onehot, counts, 0.0), axis=1).astype(jnp.int32)
    slot = (flat_route * capacity + rank).reshape(tokens, top)
    slot_id = jnp.arange(all_experts * capacity, dtype=jnp.int32)
    match = slot_id[:, None, None] == slot[None, :, :]
    chosen = jnp.any(match, axis=2).astype(bf16)
    slot_weight = jnp.sum(jnp.where(match, route_weight[None], 0.0), axis=(1, 2))
    pick = (
        jnp.any(
            slot_id.reshape(seq, experts, 1, capacity, 1) == slot[None, None, :, None, :], axis=4
        )
    ).astype(bf16)
    own_input = lax.dynamic_slice_in_dim(layer_input, column, width, 1)
    own_cot = lax.dynamic_slice_in_dim(cotangent, column, width, 1)
    block_shape = (seq, experts, capacity, width)
    rows_send = jnp.dot(chosen, own_input, preferred_element_type=f32).astype(bf16)
    cot_send = (
        slot_weight[:, None] * jnp.dot(chosen, own_cot, preferred_element_type=f32)
    ).astype(bf16)

    expert_shape = jax.ShapeDtypeStruct((experts, seq, capacity, model), bf16)
    expert_rows, weighted, total_all, kv_all = call(
        functools.partial(dispatch_kernel, seq, tensor, width),
        (
            expert_shape,
            expert_shape,
            jax.ShapeDtypeStruct((seq, heads, DK), f32),
            jax.ShapeDtypeStruct((seq, heads, DK, DV), bf16),
        ),
        (VMEM, VMEM, VMEM, VMEM),
        (ANY, ANY, VMEM, VMEM),
        [
            dma((2, seq)),
            dma((2, seq)),
            dma((3, 2, seq)),
            dma((3, 2, seq)),
            dma((2, seq)),
            dma((2, seq)),
            dma((4,)),
        ],
        0,
    )(rows_send.reshape(block_shape), cot_send.reshape(block_shape), total, kv_send)
    expert_rows = expert_rows.reshape(experts, seq * capacity, model)
    weighted = weighted.reshape(experts, seq * capacity, model)

    pre_gate = jnp.einsum("erd,edf->erf", expert_rows, gate_weight, preferred_element_type=f32)
    pre_up = jnp.einsum("erd,edf->erf", expert_rows, up_weight, preferred_element_type=f32)
    d_act = jnp.einsum("erd,efd->erf", weighted, down_weight, preferred_element_type=f32)
    sigmoid_gate = jax.nn.sigmoid(pre_gate)
    silu_gate = pre_gate * sigmoid_gate
    act = (silu_gate * pre_up).astype(bf16)
    d_gate = (d_act * pre_up * sigmoid_gate * (1.0 + pre_gate * (1.0 - sigmoid_gate))).astype(bf16)
    d_up = (d_act * silu_gate).astype(bf16)
    partial_value = (
        jnp.einsum("erf,edf->erd", d_gate, gate_weight, preferred_element_type=f32)
        + jnp.einsum("erf,edf->erd", d_up, up_weight, preferred_element_type=f32)
    ).astype(bf16)
    grad_gate, grad_up, grad_down = (
        jnp.einsum("erd,erf->edf", expert_rows, d_gate, preferred_element_type=f32),
        jnp.einsum("erd,erf->edf", expert_rows, d_up, preferred_element_type=f32),
        jnp.einsum("erf,erd->efd", act, weighted, preferred_element_type=f32),
    )

    token_parts, mixed_all = call(
        functools.partial(return_kernel, seq, tensor, width),
        (
            jax.ShapeDtypeStruct((tensor, tokens, width), bf16),
            jax.ShapeDtypeStruct((seq,) + mixed_heads.shape, bf16),
        ),
        (VMEM, VMEM, VMEM, VMEM),
        (VMEM, ANY),
        [
            pltpu.VMEM((tensor - 1,) + block_shape, bf16),
            pltpu.VMEM(block_shape, bf16),
            pltpu.VMEM(block_shape, bf16),
            pltpu.VMEM((tokens, width), f32),
            dma((tensor - 1, seq)),
            dma((tensor - 1, seq)),
            dma((seq,)),
            dma((seq,)),
            dma((seq,)),
            dma((seq,)),
            dma((3,)),
            dma((3,)),
            dma,
        ],
        1,
    )(
        partial_value.reshape(experts, seq, capacity, model),
        own_cot,
        pick,
        mixed_heads,
    )
    token_grad = jnp.transpose(token_parts, (1, 0, 2)).reshape(tokens, model)
    head_grad = lax.dot_general(
        token_grad, out_proj, (((1,), (1,)), ((), ())), preferred_element_type=f32
    )
    grad_f = head_grad.reshape(tokens, heads, DV)
    qo_bwd = jnp.einsum("thc,thv->hcv", query_f * tail, grad_f, precision=high)
    qo_fwd = jnp.einsum("thc,thv->hcv", query_f * head_part, grad_f, precision=high)
    qo_send = jnp.stack([qo_bwd, qo_fwd]).astype(bf16)
    share = model // seq
    token_send = jnp.transpose(token_grad.reshape(tokens, seq, share), (1, 0, 2))
    qo_all, token_all = call(
        functools.partial(exchange_kernel, seq, tensor),
        (
            jax.ShapeDtypeStruct((seq, heads, DK, DV), bf16),
            jax.ShapeDtypeStruct((seq, tokens, share), bf16),
        ),
        (VMEM, VMEM),
        (VMEM, VMEM),
        [dma((2, seq)), dma((2, seq)), dma((2,))],
        2,
    )(qo_send, token_send)
    grad_proj = lax.dot_general(
        token_all, mixed_all, (((0, 1), (0, 1)), ((), ())), preferred_element_type=f32
    )

    pair = jnp.einsum("thv,shv->hts", grad_f, value_f, precision=high)
    parts = local_parts(query_f, key_f, grad_f, pair, decays)
    block = jnp.arange(seq, dtype=jnp.int32)
    low_span = ((block[None, :] > block[:, None]) & (block[None, :] < s)).astype(f32)
    high_span = ((block[None, :] < block[:, None]) & (block[None, :] > s)).astype(f32)

    def carry(span, mask):
        logs = jnp.sum(span[:, :, None, None] * total_all[None], axis=1)
        return jnp.where(mask[:, None, None], jnp.exp(logs), 0.0)[..., None]

    low_scale = carry(low_span, block < s)
    high_scale = carry(high_span, block > s)
    kv_low = jnp.sum(low_scale * kv_all.astype(f32), axis=0)
    kv_high = jnp.sum(high_scale * kv_all.astype(f32), axis=0)
    qo_low = jnp.sum(low_scale * qo_all.astype(f32), axis=0)
    qo_high = jnp.sum(high_scale * qo_all.astype(f32), axis=0)
    query_grad, key_grad, value_grad, grad_cum = carried(
        parts, (kv_low, qo_low, qo_high, kv_high), query_f, key_f, value_f, grad_f
    )
    decay_all = jnp.exp(total)[..., None]
    beyond = DK ** (-0.5) * jnp.sum(
        (decay_all * kv_low + kv_fwd) * qo_high + (decay_all * qo_low + qo_bwd) * kv_high, axis=2
    )
    grad_decay = tail_sum(grad_cum) + beyond[None]
    return (
        grad_gate,
        grad_up,
        grad_down,
        grad_proj,
        query_grad.reshape(tokens, heads * DK),
        key_grad.reshape(tokens, heads * DK),
        value_grad.reshape(tokens, heads * DV),
        grad_decay.reshape(tokens, heads * DK),
    )


def solution(mesh):
    return jax.shard_map(
        body,
        mesh=mesh,
        in_specs=(
            P("sp", "tp"),
            P("sp", "tp"),
            P("sp", "tp"),
            P("sp", "tp"),
            P("sp", "tp"),
            P("tp", None),
            P("sp", None),
            P("sp", None),
            P("sp", None),
            P("sp", None),
            P("sp", None, "tp"),
            P("sp", None, "tp"),
            P("sp", "tp", None),
        ),
        out_specs=(
            P("sp", None, "tp"),
            P("sp", None, "tp"),
            P("sp", "tp", None),
            P("sp", "tp"),
            P("sp", "tp"),
            P("sp", "tp"),
            P("sp", "tp"),
            P("sp", "tp"),
        ),
        check_vma=False,
    )
```
